32 devices in a mesh: gr: 2 (over x), sp: 8 (over z, y), tp: 2 (over core).
Axes of the slice: x: 2, y: 2, z: 4, core: 2. Of those that a mesh axis runs over, the one named last changes fastest.
Arguments:
- tokens: bfloat16 [4, 4096, 2048], P('gr', 'sp'), parts along dimension 0, may hold values from -6 to 6
- key_matrix: bfloat16 [2048, 2048], P(None, 'tp'), may hold values from -0.125 to 0.125
- value_matrix: bfloat16 [2048, 2048], P(None, 'tp'), may hold values from -0.125 to 0.125
- gate_matrix: bfloat16 [2048, 16], replicated, may hold values from -0.125 to 0.125
- decay_matrix: bfloat16 [2048, 16], replicated, may hold values from -0.125 to 0.125
- gate_bias_offset: float32 [16], replicated, may hold values from -8 to 1
- head_log_decay_rate: float32 [16], replicated, may hold values from -12 to -2
- extra_log_decay: float32 [4, 4096, 16], P('gr', 'sp', 'tp'), parts along dimension 0, may hold values from -1 to 0
- next_token_query: bfloat16 [4, 16, 128], P('gr', 'tp'), parts along dimension 0, may hold values from -6 to 6
- next_token_key: bfloat16 [4, 16, 128], P('gr', 'tp'), parts along dimension 0, may hold values from -6 to 6
- next_token_value: bfloat16 [4, 16, 128], P('gr', 'tp'), parts along dimension 0, may hold values from -6 to 6
- next_token_gate: float32 [4, 16], P('gr', 'tp'), parts along dimension 0, may hold values from -2 to 2
- readout_norm_gain: float32 [128], replicated, may hold values from 0.1 to 1.9
Outputs:
- state_cache: bfloat16 [4, 16, 128, 128], P('gr', 'tp', 'sp'), parts along dimension 0
- first_read: bfloat16 [4, 16, 128], P('gr', 'tp'), parts along dimension 0
The draws below stay inside these ranges and needn't reach their ends.
There are 2 independent parts, one for each index of `gr`. The reference program is written for one: setup_inputs(seed, part) draws one part's arguments, and reference() takes and returns one part's arrays. A program takes and returns all parts, laid end to end along the dimension named above; an argument that names none is the same for every part. Nothing has to cross between parts.
All inputs are finite; a program needn't handle non-finite values.
Results may differ from the reference program's by a relative error of at most 0.009.
Values sent between devices are 32-bit elements; how exact they have to be, the bound alone decides.
A program may use at most 64 MiB of HBM per device.

```python
import math
import jax
import jax.numpy as jnp
from jax import lax

D = 2048
H = 16
DK = 128
BLOCK = 64
GROUP_SEQUENCES = 2
SEG = 512
SEQUENCE_LENGTH = 4096


def head_ranking(key):
    return jax.random.permutation(jax.random.fold_in(key, 101), H)


def draw_head_log_decay_rate(key, part):
    ranking = head_ranking(key)
    slow_mask = ranking < H // 2
    spread = jax.random.uniform(jax.random.fold_in(key, 5), (H,), jnp.float32, -0.4, 0.4)
    slow_rate = math.log(0.5 / (0.7 * SEQUENCE_LENGTH)) + spread
    fast_rate = math.log(1.0 / 28.0) + 0.75 * spread
    return jnp.where(slow_mask, slow_rate, fast_rate).astype(jnp.float32)


def draw_gate_bias_offset(key, part):
    ranking = head_ranking(key)
    slow_mask = ranking < H // 2
    shake = jax.random.uniform(jax.random.fold_in(key, 7), (H,), jnp.float32, -0.5, 0.5)
    slow_shift = math.log(DK / (8.0 * SEQUENCE_LENGTH)) + shake
    fast_shift = 2.0 * shake
    return jnp.where(slow_mask, slow_shift, fast_shift).astype(jnp.float32)


def draw_extra_log_decay(key, part):
    steady_rate = jnp.exp(jax.random.uniform(jax.random.fold_in(key, 11), (GROUP_SEQUENCES, SEQUENCE_LENGTH // SEG, 1, H), jnp.float32, math.log(0.1), 0.0)) / SEQUENCE_LENGTH
    steady_rate = jnp.broadcast_to(steady_rate, (GROUP_SEQUENCES, SEQUENCE_LENGTH // SEG, SEG, H)).reshape(GROUP_SEQUENCES, SEQUENCE_LENGTH, H)
    spike_positions = jax.random.randint(jax.random.fold_in(key, 13), (GROUP_SEQUENCES, 2), 0, SEQUENCE_LENGTH)
    spike_mask = jnp.any(jnp.arange(SEQUENCE_LENGTH)[None, :, None] == spike_positions[:, None, :], axis=-1)
    write_strength = jnp.log(jax.random.uniform(jax.random.fold_in(key, 17), (GROUP_SEQUENCES, SEQUENCE_LENGTH, H), jnp.float32, 0.55, 0.8))
    return (jnp.where(spike_mask[..., None], write_strength, 0.0) - steady_rate).astype(jnp.float32)


def levels(own_key, dims, shards, least, high):
    factor_of = 1.0
    for axis_at, shards_of in shards:
        heights = jax.random.uniform(jax.random.fold_in(jax.random.fold_in(own_key, 6), axis_at), (shards_of,), jnp.float32, least / len(shards), high / len(shards))
        factor_of = factor_of * jnp.repeat(jnp.exp(heights), dims[axis_at] // shards_of).reshape((-1,) + (1,) * (len(dims) - 1 - axis_at))
    return factor_of


def normal_values(stream_key, extent, deviation, reach, cuts=(), kind=jnp.bfloat16):
    gain = levels(stream_key, extent, cuts, -0.22, 0.18) if cuts else 1.0
    result = jax.random.normal(stream_key, extent, jnp.float32) * deviation * gain
    return jnp.minimum(jnp.maximum(result, -reach), reach).astype(kind)


def setup_inputs(seed: int = 0, part: int = 0) -> dict:
    keys = jax.random.split(jax.random.key(seed), 14)
    part_keys = jax.random.split(jax.random.fold_in(keys[13], part), 14)
    tokens = normal_values(part_keys[0], (GROUP_SEQUENCES, SEQUENCE_LENGTH, D), 1.0, 6.0, ((1, 8),))
    key_matrix = normal_values(keys[1], (D, H * DK), D ** -0.5, 0.125, ((1, 2),))
    value_matrix = normal_values(keys[2], (D, H * DK), D ** -0.5, 0.125, ((1, 2),))
    gate_matrix = normal_values(keys[3], (D, H), D ** -0.5, 0.125)
    decay_matrix = normal_values(keys[4], (D, H), D ** -0.5, 0.125)
    gate_bias_offset = draw_gate_bias_offset(jax.random.fold_in(keys[13], 71), part)
    head_log_decay_rate = draw_head_log_decay_rate(jax.random.fold_in(keys[13], 71), part)
    extra_log_decay = draw_extra_log_decay(jax.random.fold_in(jax.random.fold_in(keys[13], part), 71), part)
    next_token_query = normal_values(part_keys[8], (GROUP_SEQUENCES, H, DK), 1.0, 6.0, ((1, 2),))
    next_token_key = normal_values(part_keys[9], (GROUP_SEQUENCES, H, DK), 1.0, 6.0, ((1, 2),))
    next_token_value = normal_values(part_keys[10], (GROUP_SEQUENCES, H, DK), 1.0, 6.0, ((1, 2),))
    next_token_gate = jnp.clip(jax.random.uniform(part_keys[11], (GROUP_SEQUENCES, H), jnp.float32, -2.0, 2.0) * levels(part_keys[11], (GROUP_SEQUENCES, H), ((1, 2),), -0.4, 0.0), -2.0, 2.0)
    readout_norm_gain = jnp.clip(1.0 + 0.18 * jax.random.normal(keys[12], (DK,), jnp.float32), 0.1, 1.9)
    return dict(tokens=tokens, key_matrix=key_matrix, value_matrix=value_matrix, gate_matrix=gate_matrix, decay_matrix=decay_matrix, gate_bias_offset=gate_bias_offset, head_log_decay_rate=head_log_decay_rate, extra_log_decay=extra_log_decay, next_token_query=next_token_query, next_token_key=next_token_key, next_token_value=next_token_value, next_token_gate=next_token_gate, readout_norm_gain=readout_norm_gain)


def unit_rows(array):
    return array * lax.rsqrt(lax.optimization_barrier(jnp.sum(array * array, axis=-1, keepdims=True)) + 1e-06)

def exact_matmul(left, right):
    return jnp.matmul(left, right, precision=lax.Precision.HIGHEST)

def to_blocks(array, block_len):
    seq_count, length, head_count = array.shape[:3]
    tail_dims = array.shape[3:]
    split_view = array.reshape((seq_count, length // block_len, block_len, head_count) + tail_dims)
    axes_order = (1, 0, 3, 2) + tuple(range(4, split_view.ndim))
    return jnp.transpose(split_view, axes_order)

def block_terms(key_rows, value_rows, beta_rows, decay_logarithm):
    block_len = key_rows.shape[-2]
    cumulative = jnp.cumsum(decay_logarithm, axis=-1)
    positions = jnp.arange(block_len)
    inclusive = positions[:, None] >= positions[None, :]
    strictly = positions[:, None] > positions[None, :]
    decay_mat = jnp.exp(jnp.where(inclusive, cumulative[..., :, None] - cumulative[..., None, :], -jnp.inf))
    weighted = key_rows * beta_rows[..., None]
    lower_part = jnp.where(strictly, jnp.einsum('...id,...jd->...ij', weighted, key_rows, precision=lax.Precision.HIGHEST) * decay_mat, 0.0)
    identity = jnp.eye(block_len, dtype=jnp.float32)
    power_term = -lower_part
    inverse = identity + power_term
    for _ in range(block_len.bit_length() - 2):
        power_term = exact_matmul(power_term, power_term)
        inverse = exact_matmul(inverse, identity + power_term)
    fresh_part = exact_matmul(inverse, value_rows * beta_rows[..., None])
    pull_part = exact_matmul(inverse, weighted * jnp.exp(cumulative)[..., None])
    last_cum = cumulative[..., -1:]
    outward = key_rows * jnp.exp(last_cum - cumulative)[..., None]
    carry_decay = jnp.exp(last_cum)
    return (fresh_part, pull_part, outward, carry_decay)

def advance(state_mat, pieces):
    fresh_part, pull_part, outward, carry_decay = pieces
    update = fresh_part - jnp.einsum('shck,shkv->shcv', pull_part, state_mat, precision=lax.Precision.HIGHEST)
    state_mat = state_mat * carry_decay[..., None] + jnp.einsum('shck,shcv->shkv', outward, update, precision=lax.Precision.HIGHEST)
    return (state_mat, None)

def reference(tokens, key_matrix, value_matrix, gate_matrix, decay_matrix, gate_bias_offset, head_log_decay_rate, extra_log_decay, next_token_query, next_token_key, next_token_value, next_token_gate, readout_norm_gain):
    flat = tokens.reshape(GROUP_SEQUENCES * SEQUENCE_LENGTH, D)
    key_proj = jnp.dot(flat, key_matrix, preferred_element_type=jnp.float32)
    value_proj = jnp.dot(flat, value_matrix, preferred_element_type=jnp.float32)
    key_rows = unit_rows(jax.nn.silu(key_proj).reshape(GROUP_SEQUENCES, SEQUENCE_LENGTH, H, DK)).astype(jnp.bfloat16)
    value_rows = jax.nn.silu(value_proj).reshape(GROUP_SEQUENCES, SEQUENCE_LENGTH, H, DK).astype(jnp.bfloat16)
    gate_pre = jnp.dot(flat, gate_matrix, preferred_element_type=jnp.float32).reshape(GROUP_SEQUENCES, SEQUENCE_LENGTH, H)
    decay_logits = jnp.dot(flat, decay_matrix, preferred_element_type=jnp.float32).reshape(GROUP_SEQUENCES, SEQUENCE_LENGTH, H)
    beta_rows = jax.nn.sigmoid(gate_pre + gate_bias_offset)
    decay_logarithm = -jnp.exp(head_log_decay_rate) * jax.nn.softplus(decay_logits) + extra_log_decay
    pieces = block_terms(to_blocks(key_rows.astype(jnp.float32), BLOCK), to_blocks(value_rows.astype(jnp.float32), BLOCK), to_blocks(beta_rows, BLOCK), to_blocks(decay_logarithm, BLOCK))
    start_state = jnp.zeros((GROUP_SEQUENCES, H, DK, DK), jnp.float32)
    final, _ = lax.scan(advance, start_state, pieces)
    query_unit = unit_rows(next_token_query.astype(jnp.float32))
    key_unit = unit_rows(next_token_key.astype(jnp.float32))
    beta_new = jax.nn.sigmoid(next_token_gate)
    value_new = next_token_value.astype(jnp.float32)
    key_read = jnp.einsum('shk,shkv->shv', key_unit, final, precision=lax.Precision.HIGHEST)
    query_read = jnp.einsum('shk,shkv->shv', query_unit, final, precision=lax.Precision.HIGHEST)
    intersection = lax.optimization_barrier(jnp.sum(key_unit * query_unit, axis=-1))
    missing = value_new - key_read
    updated = final + beta_new[..., None, None] * key_unit[..., :, None] * missing[..., None, :]
    read_vec = (query_read + (beta_new * intersection)[..., None] * missing) / math.sqrt(DK)
    normed = read_vec * lax.rsqrt(lax.optimization_barrier(jnp.mean(read_vec * read_vec, axis=-1, keepdims=True)) + 1e-06) * readout_norm_gain
    return (updated.astype(jnp.bfloat16), normed.astype(jnp.bfloat16))
```

```python
import functools
import math

import jax
import jax.numpy as jnp
from jax import lax
from jax.experimental import pallas as pl
from jax.experimental.pallas import tpu as pltpu
from jax.sharding import PartitionSpec as P

BLOCK = 64
PACK = 4
EPS = 1e-06
F32 = jnp.float32
BF16 = jnp.bfloat16


def contract(left, right, left_dim, right_dim):
    return lax.dot_general(
        left, right, (((left_dim,), (right_dim,)), ((), ())), preferred_element_type=F32
    )


def dot(left, right):
    return contract(left, right, 1, 0)


def split(array, terms):
    pieces = []
    rest = array
    for _ in range(terms):
        piece = rest.astype(BF16)
        pieces.append(piece)
        rest = rest - piece.astype(F32)
    return pieces


def dot3(left, right):
    left_hi, left_lo = split(left, 2)
    right_hi, right_lo = split(right, 2)
    return dot(left_hi, right_hi) + (dot(left_hi, right_lo) + dot(left_lo, right_hi))


def exact_times_ones(array, ones):
    total = None
    for piece in split(array, 3):
        term = dot(piece, ones)
        total = term if total is None else total + term
    return total


def prepare(tok_ref, wgd_ref, shift_ref, rate_ref, extra_ref, rows_ref, cols_ref, masks_ref):
    heads = shift_ref.shape[0]
    length = tok_ref.shape[0]
    span = PACK * BLOCK
    row = lax.broadcasted_iota(jnp.int32, (span, span), 0)
    col = lax.broadcasted_iota(jnp.int32, (span, span), 1)
    same = (row // BLOCK) == (col // BLOCK)
    level = 0
    size = 2
    while size < BLOCK:
        inside = (row // (2 * size) == col // (2 * size)) & (row // size != col // size) & (row > col)
        masks_ref[level] = jnp.where(inside, 1.0, 0.0).astype(BF16)
        size *= 2
        level += 1
    masks_ref[level] = jnp.where(same, 1.0, 0.0).astype(BF16)
    upper = jnp.where(same & (row <= col), 1.0, 0.0).astype(BF16)
    every = jnp.where(same, 1.0, 0.0).astype(BF16)
    logits = contract(wgd_ref[...], tok_ref[...], 1, 1)
    gate = logits[:heads] + shift_ref[...]
    decay = logits[heads : 2 * heads]
    beta = 1.0 / (1.0 + jnp.exp(-gate))
    soft = jnp.maximum(decay, 0.0) + jnp.log1p(jnp.exp(-jnp.abs(decay)))
    log_decay = -jnp.exp(rate_ref[...]) * soft + extra_ref[...]
    for at in range(length // span):
        lanes = slice(at * span, (at + 1) * span)
        part = log_decay[:, lanes]
        cum = exact_times_ones(part, upper)
        total = exact_times_ones(part, every)
        grow = jnp.exp(cum)
        outward = jnp.exp(total - cum)
        carry = jnp.exp(total)
        b = beta[:, lanes]
        for h in range(heads):
            one = slice(h, h + 1)
            stack = jnp.concatenate(
                [cum[one], b[one], b[one] * grow[one], outward[one], carry[one],
                 cum[one], cum[one], cum[one]],
                axis=0,
            )
            rows_ref[h, :, lanes] = stack
            cols_ref[h, lanes, :] = jnp.transpose(stack)


def pack_terms(keys, values, rows, cols, masks_ref):
    span = PACK * BLOCK
    levels = masks_ref.shape[0] - 1
    row = lax.broadcasted_iota(jnp.int32, (span, span), 0)
    col = lax.broadcasted_iota(jnp.int32, (span, span), 1)
    strict = (row // BLOCK == col // BLOCK) & (row > col)
    cum_col, beta_col, pull_col, out_col = (cols[:, i : i + 1] for i in range(4))
    cum_row = rows[0:1]
    gram = contract(keys, keys, 1, 1)
    scale = jnp.exp(jnp.where(strict, cum_col - cum_row, -1e30))
    lower = (beta_col * gram) * scale
    packed = lower[0:BLOCK]
    for p in range(1, PACK):
        packed = packed + lower[p * BLOCK : (p + 1) * BLOCK]
    lower = lower.astype(BF16)
    prow = lax.broadcasted_iota(jnp.int32, (BLOCK, span), 0)
    pcol = lax.rem(lax.broadcasted_iota(jnp.int32, (BLOCK, span), 1), BLOCK)
    inv = jnp.where(prow == pcol, 1.0, jnp.where(prow // 2 == pcol // 2, -packed, 0.0))
    block_mask = masks_ref[levels]
    for level in range(levels):
        inv_bf = inv.astype(BF16)
        inv_full = jnp.concatenate([inv_bf] * PACK, axis=0) * block_mask
        left = dot(inv_bf, lower * masks_ref[level])
        inv = inv - dot(left.astype(BF16), inv_full)
    inv_bf = inv.astype(BF16)
    inv_full = jnp.concatenate([inv_bf] * PACK, axis=0) * block_mask
    keys_f = keys.astype(F32)
    right = jnp.concatenate(
        [(-(pull_col * keys_f)).astype(BF16), (beta_col * values).astype(BF16)], axis=1
    )
    fresh = dot(inv_full, right).astype(BF16)
    outward = (keys_f * out_col).astype(BF16)
    result = []
    for p in range(PACK):
        block = slice(p * BLOCK, (p + 1) * BLOCK)
        carry = rows[4:5, p * BLOCK : p * BLOCK + 1]
        result.append((carry, contract(outward[block], fresh[block], 0, 0)))
    return result


def join(earlier, later):
    early_carry, early = earlier
    late_carry, late = later
    size = early.shape[0]
    grown = dot(late[:, :size].astype(BF16), early.astype(BF16))
    rest = jnp.concatenate([early_carry * late[:, :size], late[:, size:]], axis=1)
    return (early_carry * late_carry, late_carry * early + grown + rest)


def segment_kernel(
    seqs, dim, tok_ref, wk_ref, wv_ref, wgd_ref, shift_ref, rate_ref, extra_ref,
    out_ref, rows_ref, cols_ref, masks_ref, key_ref, value_ref,
):
    step = pl.program_id(0)

    @pl.when(step == 0)
    def _():
        prepare(tok_ref, wgd_ref, shift_ref, rate_ref, extra_ref, rows_ref, cols_ref, masks_ref)

    length = tok_ref.shape[0] // seqs
    per_step = wk_ref.shape[1] // dim
    span = PACK * BLOCK
    key_ref[...] = dot(tok_ref[...], wk_ref[...])
    value_ref[...] = dot(tok_ref[...], wv_ref[...])
    eye = lax.broadcasted_iota(jnp.int32, (dim, dim), 0) == lax.broadcasted_iota(
        jnp.int32, (dim, dim), 1
    )
    for j in range(per_step):
        head = step * per_step + j
        for s in range(seqs):
            terms = []
            for at in range(length // span):
                lanes = slice(s * length + at * span, s * length + (at + 1) * span)
                heads = slice(j * dim, (j + 1) * dim)
                key = key_ref[lanes, heads]
                key = key / (1.0 + jnp.exp(-key))
                key = key * lax.rsqrt(jnp.sum(key * key, axis=-1, keepdims=True) + EPS)
                value = value_ref[lanes, heads]
                value = (value / (1.0 + jnp.exp(-value))).astype(BF16).astype(F32)
                terms += pack_terms(
                    key.astype(BF16), value, rows_ref[head, :, lanes],
                    cols_ref[head, lanes, :], masks_ref,
                )
            while len(terms) > 1:
                terms = [join(terms[i], terms[i + 1]) for i in range(0, len(terms), 2)]
            carry, both = terms[0]
            diagonal = jnp.where(eye, carry, 0.0)
            out_ref[j * seqs + s, :, :dim] = both[:, :dim] + diagonal
            out_ref[j * seqs + s, :, dim:] = both[:, dim:]


def segment_maps(flat, key_matrix, value_matrix, wgd, shift, rate, extra, seqs, heads, dim):
    rows, width = flat.shape
    per_step = 2 if heads % 2 == 0 else 1
    span = PACK * BLOCK
    levels = BLOCK.bit_length() - 2
    whole = lambda shape: pl.BlockSpec(shape, lambda g: (0,) * len(shape))
    return pl.pallas_call(
        functools.partial(segment_kernel, seqs, dim),
        grid=(heads // per_step,),
        in_specs=[
            whole((rows, width)),
            pl.BlockSpec((width, per_step * dim), lambda g: (0, g)),
            pl.BlockSpec((width, per_step * dim), lambda g: (0, g)),
            whole(wgd.shape),
            whole(shift.shape),
            whole(rate.shape),
            whole(extra.shape),
        ],
        out_specs=pl.BlockSpec((per_step * seqs, dim, 2 * dim), lambda g: (g, 0, 0)),
        out_shape=jax.ShapeDtypeStruct((heads * seqs, dim, 2 * dim), F32),
        scratch_shapes=[
            pltpu.VMEM((heads, 8, rows), F32),
            pltpu.VMEM((heads, rows, 8), F32),
            pltpu.VMEM((levels + 1, span, span), BF16),
            pltpu.VMEM((rows, per_step * dim), F32),
            pltpu.VMEM((rows, per_step * dim), F32),
        ],
        compiler_params=pltpu.CompilerParams(
            dimension_semantics=("arbitrary",), vmem_limit_bytes=60 * 1024 * 1024
        ),
    )(flat, key_matrix, value_matrix, wgd, shift, rate, extra)


def token_step(final, info, gain):
    query, key, value, gate = (info[i : i + 1] for i in range(4))
    query = query * lax.rsqrt(jnp.sum(query * query, axis=-1, keepdims=True) + EPS)
    key = key * lax.rsqrt(jnp.sum(key * key, axis=-1, keepdims=True) + EPS)
    beta = 1.0 / (1.0 + jnp.exp(-gate))
    columns = jnp.transpose(jnp.concatenate([key, query, key * beta, key] + [key] * 4, axis=0))
    key_read = jnp.sum(columns[:, 0:1] * final, axis=0, keepdims=True)
    query_read = jnp.sum(columns[:, 1:2] * final, axis=0, keepdims=True)
    missing = value - key_read
    updated = final + columns[:, 2:3] * missing
    cross = jnp.sum(key * query, axis=-1, keepdims=True)
    read = (query_read + beta * cross * missing) / math.sqrt(final.shape[-1])
    read = read * lax.rsqrt(jnp.mean(read * read, axis=-1, keepdims=True) + EPS) * gain
    return updated, read


def first_pair(place, count, devices):
    start = 0
    bit = 1
    left = count
    while bit < devices:
        left //= 2
        start = start + lax.rem(place // bit, 2) * left if not isinstance(place, int) else (
            start + (place // bit) % 2 * left
        )
        bit *= 2
    return start


def exchange_kernel(
    devices, seqs, ab_ref, info_ref, gain_ref, state_ref, read_ref,
    got_ref, made_ref, out_buf, in_buf, read_buf, send_sem, recv_sem, put_sem, get_sem,
):
    me = lax.axis_index("sp")
    count, dim = ab_ref.shape[0], ab_ref.shape[1]
    barrier = pltpu.get_barrier_semaphore()
    for k in range(1, devices):
        pl.semaphore_signal(
            barrier, inc=1, device_id={"sp": lax.rem(me + k, devices)},
            device_id_type=pl.DeviceIdType.MESH,
        )
    pl.semaphore_wait(barrier, devices - 1)

    levels = devices.bit_length() - 1

    def halves(level):
        size = count >> (level + 1)
        bit = lax.rem(me // (1 << level), 2)
        return size, bit, bit * size, (1 - bit) * size

    def source(level, at):
        if level == 0:
            return ab_ref.at[at]
        return made_ref.at[made_base(level) + at]

    def made_base(level):
        return sum(count >> i for i in range(1, level))

    def copy(level, i):
        size, bit, keep, give = halves(level)
        slot = made_base(level + 1) + i
        partner = me + (1 - 2 * bit) * (1 << level)
        return pltpu.make_async_remote_copy(
            src_ref=source(level, give + i), dst_ref=got_ref.at[slot],
            send_sem=send_sem.at[slot], recv_sem=recv_sem.at[slot],
            device_id={"sp": partner}, device_id_type=pl.DeviceIdType.MESH,
        )

    for i in range(count // 2):
        copy(0, i).start()
    for level in range(levels):
        size, bit, keep, give = halves(level)
        base = made_base(level + 1)
        last = level == levels - 1
        if not last:
            nsize, nbit, nkeep, ngive = halves(level + 1)
        for i in range(size):
            if last:
                at = i
            elif i < nsize:
                at = ngive + i
            else:
                at = nkeep + (i - nsize)
            size_, bit_, keep_, give_ = size, bit, keep, give
            slot = base + at
            pltpu.make_async_remote_copy(
                src_ref=source(level, give + at), dst_ref=got_ref.at[slot],
                send_sem=send_sem.at[slot], recv_sem=recv_sem.at[slot],
                device_id={"sp": me + (1 - 2 * bit) * (1 << level)},
                device_id_type=pl.DeviceIdType.MESH,
            ).wait()
            mine = source(level, keep + at)[...]
            theirs = got_ref[slot]
            is_late = bit == 1
            late = jnp.where(is_late, mine, theirs)
            early = jnp.where(is_late, theirs, mine)
            late_map, late_add = late[:, :dim], late[:, dim:]
            if last:
                final = dot3(late_map, early[:, dim:]) + late_add
                pair = first_pair(me, count, devices) + i
                updated, read = token_step(final, info_ref[pair], gain_ref[...])
                out_buf[:, i, : dim // devices, :] = updated.reshape(devices, dim // devices, dim)
                out_buf[:, i, dim // devices :, :] = jnp.broadcast_to(read, (devices, 8, dim))
            else:
                grown = dot3(late_map, early)
                made_ref[slot, :, :dim] = grown[:, :dim]
                made_ref[slot, :, dim:] = grown[:, dim:] + late_add
                if i < nsize:
                    copy(level + 1, i).start()

    def put(k):
        dest = lax.rem(me + k, devices)
        return pltpu.make_async_remote_copy(
            src_ref=out_buf.at[dest], dst_ref=in_buf.at[me],
            send_sem=put_sem.at[k], recv_sem=get_sem.at[k],
            device_id={"sp": dest}, device_id_type=pl.DeviceIdType.MESH,
        )

    for k in range(1, devices):
        put(k).start()
    in_buf[me] = out_buf[me]
    for k in range(1, devices):
        put(k).wait()
    own = count // devices
    rows = dim // devices
    for e in range(devices):
        for i in range(own):
            pair = first_pair(e, count, devices) + i
            h, s = pair // seqs, pair % seqs
            state_ref[s, h] = in_buf[e, i, :rows, :].astype(BF16)
            read_buf[s, h : h + 1, :] = in_buf[e, i, rows : rows + 1, :]
    read_ref[...] = read_buf[...].astype(BF16)


def exchange(ab, info, gain, seqs, heads, devices):
    count, dim = ab.shape[0], ab.shape[1]
    slots = count - count // devices
    vmem = pl.BlockSpec(memory_space=pltpu.VMEM)
    return pl.pallas_call(
        functools.partial(exchange_kernel, devices, seqs),
        in_specs=[vmem] * 3,
        out_specs=[vmem] * 2,
        out_shape=[
            jax.ShapeDtypeStruct((seqs, heads, dim // devices, dim), BF16),
            jax.ShapeDtypeStruct((seqs, heads, dim), BF16),
        ],
        scratch_shapes=[
            pltpu.VMEM((slots, dim, 2 * dim), F32),
            pltpu.VMEM((slots, dim, 2 * dim), F32),
            pltpu.VMEM((devices, count // devices, dim // devices + 8, dim), F32),
            pltpu.VMEM((devices, count // devices, dim // devices + 8, dim), F32),
            pltpu.VMEM((seqs, heads, dim), F32),
            pltpu.SemaphoreType.DMA((slots,)),
            pltpu.SemaphoreType.DMA((slots,)),
            pltpu.SemaphoreType.DMA((devices,)),
            pltpu.SemaphoreType.DMA((devices,)),
        ],
        compiler_params=pltpu.CompilerParams(
            collective_id=0, has_side_effects=True, vmem_limit_bytes=40 * 1024 * 1024
        ),
    )(ab, info, gain)


def gathered_exchange(ab, info, gain, seqs, heads, devices):
    count, dim = ab.shape[0], ab.shape[1]
    everyone = lax.all_gather(ab, "sp")

    def one(at, state):
        step = lax.dynamic_index_in_dim(everyone, at, 0, False)
        return (
            jnp.matmul(step[..., :dim], state, precision=lax.Precision.HIGHEST) + step[..., dim:]
        )

    final = lax.fori_loop(0, devices, one, jnp.zeros((count, dim, dim), F32))
    updated, read = jax.vmap(lambda f, i: token_step(f, i, gain))(final, info)
    rows = dim // devices
    mine = lax.dynamic_slice_in_dim(updated, lax.axis_index("sp") * rows, rows, 1)
    mine = jnp.swapaxes(mine.reshape(heads, seqs, rows, dim), 0, 1)
    return mine.astype(BF16), jnp.swapaxes(read.reshape(heads, seqs, dim), 0, 1).astype(BF16)


def shards(
    tokens, key_matrix, value_matrix, gate_matrix, decay_matrix, gate_bias_offset,
    head_log_decay_rate, extra_log_decay, next_token_query, next_token_key,
    next_token_value, next_token_gate, readout_norm_gain,
):
    seqs, length, width = tokens.shape
    dim = next_token_key.shape[-1]
    heads = key_matrix.shape[1] // dim
    devices = lax.axis_size("sp")
    first = lax.axis_index("tp") * heads
    flat = tokens.reshape(seqs * length, width)
    pick = lambda array, axis: lax.dynamic_slice_in_dim(array, first, heads, axis)
    wgd = jnp.concatenate([pick(gate_matrix, 1), pick(decay_matrix, 1)], axis=1).T
    shift = pick(gate_bias_offset, 0)[:, None]
    rate = pick(head_log_decay_rate, 0)[:, None]
    extra = extra_log_decay.reshape(seqs * length, heads).T
    ab = segment_maps(
        flat, key_matrix, value_matrix, wgd, shift, rate, extra, seqs, heads, dim
    )
    wide = lambda array: jnp.swapaxes(array.astype(F32), 0, 1).reshape(heads * seqs, 1, dim)
    gate = jnp.broadcast_to(next_token_gate[..., None], next_token_key.shape)
    info = jnp.concatenate(
        [wide(next_token_query), wide(next_token_key), wide(next_token_value), wide(gate)], axis=1
    )
    gain = readout_norm_gain[None, :]
    whole = (seqs * heads) % devices == 0 and devices & (devices - 1) == 0 and devices > 1
    run = exchange if whole else gathered_exchange
    return run(ab, info, gain, seqs, heads, devices)


def solution(mesh):
    return jax.shard_map(
        shards,
        mesh=mesh,
        in_specs=(
            P("gr", "sp", None), P(None, "tp"), P(None, "tp"), P(), P(), P(), P(),
            P("gr", "sp", "tp"), P("gr", "tp", None), P("gr", "tp", None),
            P("gr", "tp", None), P("gr", "tp"), P(),
        ),
        out_specs=(P("gr", "tp", "sp", None), P("gr", "tp", None)),
        check_vma=False,
    )
```

```python
import functools
import math

import jax
import jax.numpy as jnp
from jax import lax
from jax.experimental import pallas as pl
from jax.experimental.pallas import tpu as pltpu
from jax.sharding import PartitionSpec as P

BLOCK = 64
PACK = 4
EPS = 1e-06
F32 = jnp.float32
BF16 = jnp.bfloat16


def contract(left, right, left_dim, right_dim):
    return lax.dot_general(
        left, right, (((left_dim,), (right_dim,)), ((), ())), preferred_element_type=F32
    )


def dot(left, right):
    return contract(left, right, 1, 0)


def split(array, terms):
    pieces = []
    rest = array
    for _ in range(terms):
        piece = rest.astype(BF16)
        pieces.append(piece)
        rest = rest - piece.astype(F32)
    return pieces


def dot3(left, right):
    left_hi, left_lo = split(left, 2)
    right_hi, right_lo = split(right, 2)
    return dot(left_hi, right_hi) + (dot(left_hi, right_lo) + dot(left_lo, right_hi))


def exact_times_ones(array, ones):
    total = None
    for piece in split(array, 3):
        term = dot(piece, ones)
        total = term if total is None else total + term
    return total


def prepare(tok_ref, wgd_ref, shift_ref, rate_ref, extra_ref, rows_ref, cols_ref, masks_ref):
    heads = shift_ref.shape[0]
    length = tok_ref.shape[0]
    span = PACK * BLOCK
    row = lax.broadcasted_iota(jnp.int32, (span, span), 0)
    col = lax.broadcasted_iota(jnp.int32, (span, span), 1)
    same = (row // BLOCK) == (col // BLOCK)
    level = 0
    size = 2
    while size < BLOCK:
        inside = (row // (2 * size) == col // (2 * size)) & (row // size != col // size) & (row > col)
        masks_ref[level] = jnp.where(inside, 1.0, 0.0).astype(BF16)
        size *= 2
        level += 1
    masks_ref[level] = jnp.where(same, 1.0, 0.0).astype(BF16)
    upper = jnp.where(same & (row <= col), 1.0, 0.0).astype(BF16)
    every = jnp.where(same, 1.0, 0.0).astype(BF16)
    logits = contract(wgd_ref[...], tok_ref[...], 1, 1)
    gate = logits[:heads] + shift_ref[...]
    decay = logits[heads : 2 * heads]
    beta = 1.0 / (1.0 + jnp.exp(-gate))
    soft = jnp.maximum(decay, 0.0) + jnp.log1p(jnp.exp(-jnp.abs(decay)))
    log_decay = -jnp.exp(rate_ref[...]) * soft + extra_ref[...]
    for at in range(length // span):
        lanes = slice(at * span, (at + 1) * span)
        part = log_decay[:, lanes]
        cum = exact_times_ones(part, upper)
        total = exact_times_ones(part, every)
        grow = jnp.exp(cum)
        outward = jnp.exp(total - cum)
        carry = jnp.exp(total)
        b = beta[:, lanes]
        for h in range(heads):
            one = slice(h, h + 1)
            stack = jnp.concatenate(
                [cum[one], b[one], b[one] * grow[one], outward[one], carry[one],
                 cum[one], cum[one], cum[one]],
                axis=0,
            )
            rows_ref[h, :, lanes] = stack
            cols_ref[h, lanes, :] = jnp.transpose(stack)


def pack_terms(packs, masks_ref):
    span = PACK * BLOCK
    levels = masks_ref.shape[0] - 1
    row = lax.broadcasted_iota(jnp.int32, (span, span), 0)
    col = lax.broadcasted_iota(jnp.int32, (span, span), 1)
    strict = (row // BLOCK == col // BLOCK) & (row > col)
    prow = lax.broadcasted_iota(jnp.int32, (BLOCK, span), 0)
    pcol = lax.rem(lax.broadcasted_iota(jnp.int32, (BLOCK, span), 1), BLOCK)
    unit = prow == pcol
    couple = prow // 2 == pcol // 2
    lowers, invs, rights, outwards = [], [], [], []
    for keys, values, rows, cols in packs:
        cum_col, beta_col, pull_col, out_col = (cols[:, i : i + 1] for i in range(4))
        gram = contract(keys, keys, 1, 1)
        scale = jnp.exp(jnp.where(strict, cum_col - rows[0:1], -1e30))
        lower = (beta_col * gram) * scale
        packed = lower[0:BLOCK]
        for p in range(1, PACK):
            packed = packed + lower[p * BLOCK : (p + 1) * BLOCK]
        lowers.append(lower.astype(BF16))
        invs.append(jnp.where(unit, 1.0, jnp.where(couple, -packed, 0.0)))
        keys_f = keys.astype(F32)
        rights.append(
            jnp.concatenate(
                [(-(pull_col * keys_f)).astype(BF16), (beta_col * values).astype(BF16)], axis=1
            )
        )
        outwards.append((keys_f * out_col).astype(BF16))
    block_mask = masks_ref[levels]
    widen = lambda inv: jnp.concatenate([inv] * PACK, axis=0) * block_mask
    for level in range(levels):
        mask = masks_ref[level]
        narrow = [inv.astype(BF16) for inv in invs]
        lefts = [dot(n, lower * mask).astype(BF16) for n, lower in zip(narrow, lowers)]
        invs = [inv - dot(left, widen(n)) for inv, left, n in zip(invs, lefts, narrow)]
    fresh = [
        dot(widen(inv.astype(BF16)), right).astype(BF16) for inv, right in zip(invs, rights)
    ]
    result = []
    for (_, _, rows, _), outward, new in zip(packs, outwards, fresh):
        terms = []
        for p in range(PACK):
            block = slice(p * BLOCK, (p + 1) * BLOCK)
            carry = rows[4:5, p * BLOCK : p * BLOCK + 1]
            terms.append((carry, contract(outward[block], new[block], 0, 0)))
        result.append(terms)
    return result


def join(earlier, later):
    early_carry, early = earlier
    late_carry, late = later
    size = early.shape[0]
    grown = dot(late[:, :size].astype(BF16), early.astype(BF16))
    rest = jnp.concatenate([early_carry * late[:, :size], late[:, size:]], axis=1)
    return (early_carry * late_carry, late_carry * early + grown + rest)


def silu(array):
    half = 0.5 * array
    return half + half * jnp.tanh(half)


def segment_kernel(
    seqs, dim, first_ref, tok_ref, wk_ref, wv_ref, wgd_ref, shift_ref, rate_ref, extra_ref,
    out_ref, rows_ref, cols_ref, masks_ref, key_ref, value_ref,
):
    step = pl.program_id(0)

    @pl.when(step == 0)
    def _():
        prepare(tok_ref, wgd_ref, shift_ref, rate_ref, extra_ref, rows_ref, cols_ref, masks_ref)

    length = tok_ref.shape[0] // seqs
    per_step = wk_ref.shape[1] // dim
    span = PACK * BLOCK
    key_ref[...] = dot(tok_ref[...], wk_ref[...])
    value_ref[...] = dot(tok_ref[...], wv_ref[...])
    eye = lax.broadcasted_iota(jnp.int32, (dim, dim), 0) == lax.broadcasted_iota(
        jnp.int32, (dim, dim), 1
    )
    packs = []
    for j in range(per_step):
        head = (first_ref[0] + step) * per_step + j
        heads = slice(j * dim, (j + 1) * dim)
        for at in range(seqs * length // span):
            lanes = slice(at * span, (at + 1) * span)
            key = silu(key_ref[lanes, heads])
            key = key * lax.rsqrt(jnp.sum(key * key, axis=-1, keepdims=True) + EPS)
            value = silu(value_ref[lanes, heads]).astype(BF16).astype(F32)
            packs.append(
                (key.astype(BF16), value, rows_ref[head, :, lanes], cols_ref[head, lanes, :])
            )
    terms = pack_terms(packs, masks_ref)
    each = length // span
    chains = [
        sum(terms[i * each : (i + 1) * each], []) for i in range(per_step * seqs)
    ]
    while len(chains[0]) > 1:
        chains = [
            [join(chain[i], chain[i + 1]) for i in range(0, len(chain), 2)] for chain in chains
        ]
    for i, chain in enumerate(chains):
        carry, both = chain[0]
        out_ref[i, :, :dim] = both[:, :dim] + jnp.where(eye, carry, 0.0)
        out_ref[i, :, dim:] = both[:, dim:]


def segment_maps(
    first, some, flat, key_matrix, value_matrix, wgd, shift, rate, extra, seqs, heads, dim
):
    rows, width = flat.shape
    per_step = 2 if some % 2 == 0 else 1
    span = PACK * BLOCK
    levels = BLOCK.bit_length() - 2
    whole = lambda shape: pl.BlockSpec(shape, lambda g, first: (0,) * len(shape))
    weights = pl.BlockSpec((width, per_step * dim), lambda g, first: (0, first[0] + g))
    steps = some // per_step
    return pl.pallas_call(
        functools.partial(segment_kernel, seqs, dim),
        grid_spec=pltpu.PrefetchScalarGridSpec(
            num_scalar_prefetch=1,
            grid=(steps,),
            in_specs=[
                whole((rows, width)), weights, weights, whole(wgd.shape), whole(shift.shape),
                whole(rate.shape), whole(extra.shape),
            ],
            out_specs=pl.BlockSpec(
                (per_step * seqs, dim, 2 * dim), lambda g, first: (g, 0, 0)
            ),
            scratch_shapes=[
                pltpu.VMEM((heads, 8, rows), F32),
                pltpu.VMEM((heads, rows, 8), F32),
                pltpu.VMEM((levels + 1, span, span), BF16),
                pltpu.VMEM((rows, per_step * dim), F32),
                pltpu.VMEM((rows, per_step * dim), F32),
            ],
        ),
        out_shape=jax.ShapeDtypeStruct((some * seqs, dim, 2 * dim), F32),
        compiler_params=pltpu.CompilerParams(
            dimension_semantics=("arbitrary",), vmem_limit_bytes=48 * 1024 * 1024
        ),
        cost_estimate=pl.CostEstimate(
            flops=8 * rows * width * some * dim, transcendentals=0,
            bytes_accessed=2 * rows * width + 4 * width * some * dim,
        ),
    )(first * steps, flat, key_matrix, value_matrix, wgd, shift, rate, extra)


def token_step(final, info, gain):
    query, key, value, gate = (info[i : i + 1] for i in range(4))
    query = query * lax.rsqrt(jnp.sum(query * query, axis=-1, keepdims=True) + EPS)
    key = key * lax.rsqrt(jnp.sum(key * key, axis=-1, keepdims=True) + EPS)
    beta = 1.0 / (1.0 + jnp.exp(-gate))
    columns = jnp.transpose(jnp.concatenate([key, query, key * beta, key] + [key] * 4, axis=0))
    key_read = jnp.sum(columns[:, 0:1] * final, axis=0, keepdims=True)
    query_read = jnp.sum(columns[:, 1:2] * final, axis=0, keepdims=True)
    missing = value - key_read
    updated = final + columns[:, 2:3] * missing
    cross = jnp.sum(key * query, axis=-1, keepdims=True)
    read = (query_read + beta * cross * missing) / math.sqrt(final.shape[-1])
    read = read * lax.rsqrt(jnp.mean(read * read, axis=-1, keepdims=True) + EPS) * gain
    return updated, read


def first_pair(place, count, devices):
    start = 0
    bit = 1
    left = count
    while bit < devices:
        left //= 2
        start = start + lax.rem(place // bit, 2) * left if not isinstance(place, int) else (
            start + (place // bit) % 2 * left
        )
        bit *= 2
    return start


def exchange_kernel(
    devices, seqs, ab_ref, other_ref, info_ref, gain_ref, state_ref, read_ref,
    got_ref, made_ref, out_buf, in_buf, read_buf, send_sem, recv_sem, put_sem, get_sem,
):
    me = lax.axis_index("sp")
    count, dim = 2 * ab_ref.shape[0], ab_ref.shape[1]
    barrier = pltpu.get_barrier_semaphore()
    for k in range(1, devices):
        pl.semaphore_signal(
            barrier, inc=1, device_id={"sp": lax.rem(me + k, devices)},
            device_id_type=pl.DeviceIdType.MESH,
        )
    pl.semaphore_wait(barrier, devices - 1)

    levels = devices.bit_length() - 1

    def halves(level):
        size = count >> (level + 1)
        bit = lax.rem(me // (1 << level), 2)
        return size, bit, bit * size, (1 - bit) * size

    def made_base(level):
        return sum(count >> i for i in range(1, level))

    def mine_at(level, at):
        if level == 0:
            return ab_ref[at]
        return made_ref[made_base(level) + halves(level)[2] + at]

    def order(level):
        size = count >> (level + 1)
        if level == levels - 1:
            return list(range(size))
        _, _, keep, give = halves(level + 1)
        after = order(level + 1)
        return [give + i for i in after] + [keep + i for i in after]

    def copy(level, at):
        size, bit, keep, give = halves(level)
        slot = made_base(level + 1) - count // 2 + at
        return pltpu.make_async_remote_copy(
            src_ref=made_ref.at[made_base(level) + give + at], dst_ref=got_ref.at[slot],
            send_sem=send_sem.at[slot], recv_sem=recv_sem.at[slot],
            device_id={"sp": me + (1 - 2 * bit) * (1 << level)},
            device_id_type=pl.DeviceIdType.MESH,
        )

    for level in range(levels):
        size, bit, keep, give = halves(level)
        last = level == levels - 1
        after = [] if last else order(level + 1)
        for turn, at in enumerate(order(level)):
            mine = mine_at(level, at)
            if level == 0:
                theirs = other_ref[at]
            else:
                copy(level, at).wait()
                theirs = got_ref[made_base(level + 1) - count // 2 + at]
            is_late = bit == 1
            late = jnp.where(is_late, mine, theirs)
            early = jnp.where(is_late, theirs, mine)
            late_map, late_add = late[:, :dim], late[:, dim:]
            if last:
                final = dot3(late_map, early[:, dim:]) + late_add
                pair = first_pair(me, count, devices) + at
                updated, read = token_step(final, info_ref[pair], gain_ref[...])
                out_buf[:, at, : dim // devices, :] = updated.reshape(devices, dim // devices, dim)
                out_buf[:, at, dim // devices :, :] = jnp.broadcast_to(read, (devices, 8, dim))
            else:
                grown = dot3(late_map, early)
                slot = made_base(level + 1) + at
                made_ref[slot, :, :dim] = grown[:, :dim]
                made_ref[slot, :, dim:] = grown[:, dim:] + late_add
                if turn < len(after):
                    copy(level + 1, after[turn]).start()

    def put(k):
        dest = lax.rem(me + k, devices)
        return pltpu.make_async_remote_copy(
            src_ref=out_buf.at[dest], dst_ref=in_buf.at[me],
            send_sem=put_sem.at[k], recv_sem=get_sem.at[k],
            device_id={"sp": dest}, device_id_type=pl.DeviceIdType.MESH,
        )

    for k in range(1, devices):
        put(k).start()
    in_buf[me] = out_buf[me]
    for k in range(1, devices):
        put(k).wait()
    own = count // devices
    rows = dim // devices
    for e in range(devices):
        for i in range(own):
            pair = first_pair(e, count, devices) + i
            h, s = pair // seqs, pair % seqs
            state_ref[s, h] = in_buf[e, i, :rows, :].astype(BF16)
            read_buf[s, h : h + 1, :] = in_buf[e, i, rows : rows + 1, :]
    read_ref[...] = read_buf[...].astype(BF16)


def exchange(ab, other, info, gain, seqs, heads, devices):
    count, dim = 2 * ab.shape[0], ab.shape[1]
    slots = count // 2 - count // devices
    vmem = pl.BlockSpec(memory_space=pltpu.VMEM)
    return pl.pallas_call(
        functools.partial(exchange_kernel, devices, seqs),
        in_specs=[vmem] * 4,
        out_specs=[vmem] * 2,
        out_shape=[
            jax.ShapeDtypeStruct((seqs, heads, dim // devices, dim), BF16),
            jax.ShapeDtypeStruct((seqs, heads, dim), BF16),
        ],
        scratch_shapes=[
            pltpu.VMEM((slots, dim, 2 * dim), F32),
            pltpu.VMEM((slots + count // devices + count // 2, dim, 2 * dim), F32),
            pltpu.VMEM((devices, count // devices, dim // devices + 8, dim), F32),
            pltpu.VMEM((devices, count // devices, dim // devices + 8, dim), F32),
            pltpu.VMEM((seqs, heads, dim), F32),
            pltpu.SemaphoreType.DMA((slots,)),
            pltpu.SemaphoreType.DMA((slots,)),
            pltpu.SemaphoreType.DMA((devices,)),
            pltpu.SemaphoreType.DMA((devices,)),
        ],
        compiler_params=pltpu.CompilerParams(
            collective_id=0, has_side_effects=True, vmem_limit_bytes=40 * 1024 * 1024
        ),
    )(ab, other, info, gain)


def gathered_exchange(ab, info, gain, seqs, heads, devices):
    count, dim = ab.shape[0], ab.shape[1]
    everyone = lax.all_gather(ab, "sp")

    def one(at, state):
        step = lax.dynamic_index_in_dim(everyone, at, 0, False)
        return (
            jnp.matmul(step[..., :dim], state, precision=lax.Precision.HIGHEST) + step[..., dim:]
        )

    final = lax.fori_loop(0, devices, one, jnp.zeros((count, dim, dim), F32))
    updated, read = jax.vmap(lambda f, i: token_step(f, i, gain))(final, info)
    rows = dim // devices
    mine = lax.dynamic_slice_in_dim(updated, lax.axis_index("sp") * rows, rows, 1)
    mine = jnp.swapaxes(mine.reshape(heads, seqs, rows, dim), 0, 1)
    return mine.astype(BF16), jnp.swapaxes(read.reshape(heads, seqs, dim), 0, 1).astype(BF16)


def shards(
    tokens, key_matrix, value_matrix, gate_matrix, decay_matrix, gate_bias_offset,
    head_log_decay_rate, extra_log_decay, next_token_query, next_token_key,
    next_token_value, next_token_gate, readout_norm_gain,
):
    seqs, length, width = tokens.shape
    dim = next_token_key.shape[-1]
    heads = key_matrix.shape[1] // dim
    devices = lax.axis_size("sp")
    first = lax.axis_index("tp") * heads
    flat = tokens.reshape(seqs * length, width)
    pick = lambda array, axis: lax.dynamic_slice_in_dim(array, first, heads, axis)
    wgd = jnp.concatenate([pick(gate_matrix, 1), pick(decay_matrix, 1)], axis=1).T
    shift = pick(gate_bias_offset, 0)[:, None]
    rate = pick(head_log_decay_rate, 0)[:, None]
    extra = extra_log_decay.reshape(seqs * length, heads).T
    wide = lambda array: jnp.swapaxes(array.astype(F32), 0, 1).reshape(heads * seqs, 1, dim)
    gate = jnp.broadcast_to(next_token_gate[..., None], next_token_key.shape)
    info = jnp.concatenate(
        [wide(next_token_query), wide(next_token_key), wide(next_token_value), wide(gate)], axis=1
    )
    gain = readout_norm_gain[None, :]
    maps = lambda at, some: segment_maps(
        jnp.full((1,), at, jnp.int32), some, flat, key_matrix, value_matrix, wgd, shift, rate,
        extra, seqs, heads, dim,
    )
    paired = devices & (devices - 1) == 0 and devices > 2 and heads % 2 == 0
    if not paired or (seqs * heads) % devices:
        return gathered_exchange(maps(0, heads), info, gain, seqs, heads, devices)
    late = lax.rem(lax.axis_index("sp"), 2)
    given = maps(1 - late, heads // 2)
    other = lax.ppermute(given, "sp", [(i, i ^ 1) for i in range(devices)])
    kept = maps(late, heads // 2)
    return exchange(kept, other, info, gain, seqs, heads, devices)


def solution(mesh):
    return jax.shard_map(
        shards,
        mesh=mesh,
        in_specs=(
            P("gr", "sp", None), P(None, "tp"), P(None, "tp"), P(), P(), P(), P(),
            P("gr", "sp", "tp"), P("gr", "tp", None), P("gr", "tp", None),
            P("gr", "tp", None), P("gr", "tp"), P(),
        ),
        out_specs=(P("gr", "tp", "sp", None), P("gr", "tp", None)),
        check_vma=False,
    )
```

```python
import functools
import math

import jax
import jax.numpy as jnp
from jax import lax
from jax.experimental import pallas as pl
from jax.experimental.pallas import tpu as pltpu
from jax.sharding import PartitionSpec as P

BLOCK = 64
PACK = 4
EPS = 1e-06
F32 = jnp.float32
BF16 = jnp.bfloat16


def contract(left, right, left_dim, right_dim):
    return lax.dot_general(
        left, right, (((left_dim,), (right_dim,)), ((), ())), preferred_element_type=F32
    )


def dot(left, right):
    return contract(left, right, 1, 0)


def split(array, terms):
    pieces = []
    rest = array
    for _ in range(terms):
        piece = rest.astype(BF16)
        pieces.append(piece)
        rest = rest - piece.astype(F32)
    return pieces


def dot3(left, right):
    left_hi, left_lo = split(left, 2)
    right_hi, right_lo = split(right, 2)
    return dot(left_hi, right_hi) + (dot(left_hi, right_lo) + dot(left_lo, right_hi))


def exact_times_ones(array, ones):
    total = None
    for piece in split(array, 3):
        term = dot(piece, ones)
        total = term if total is None else total + term
    return total


def prepare(tok_ref, wgd_ref, shift_ref, rate_ref, extra_ref, rows_ref, cols_ref, masks_ref):
    heads = shift_ref.shape[0]
    length = tok_ref.shape[0]
    span = PACK * BLOCK
    row = lax.broadcasted_iota(jnp.int32, (span, span), 0)
    col = lax.broadcasted_iota(jnp.int32, (span, span), 1)
    same = (row // BLOCK) == (col // BLOCK)
    level = 0
    size = 2
    while size < BLOCK:
        inside = (row // (2 * size) == col // (2 * size)) & (row // size != col // size) & (row > col)
        masks_ref[level] = jnp.where(inside, 1.0, 0.0).astype(BF16)
        size *= 2
        level += 1
    masks_ref[level] = jnp.where(same, 1.0, 0.0).astype(BF16)
    upper = jnp.where(same & (row <= col), 1.0, 0.0).astype(BF16)
    every = jnp.where(same, 1.0, 0.0).astype(BF16)
    logits = contract(wgd_ref[...], tok_ref[...], 1, 1)
    gate = logits[:heads] + shift_ref[...]
    decay = logits[heads : 2 * heads]
    beta = 1.0 / (1.0 + jnp.exp(-gate))
    soft = jnp.maximum(decay, 0.0) + jnp.log1p(jnp.exp(-jnp.abs(decay)))
    log_decay = -jnp.exp(rate_ref[...]) * soft + extra_ref[...]
    for at in range(length // span):
        lanes = slice(at * span, (at + 1) * span)
        part = log_decay[:, lanes]
        cum = exact_times_ones(part, upper)
        total = exact_times_ones(part, every)
        grow = jnp.exp(cum)
        outward = jnp.exp(total - cum)
        carry = jnp.exp(total)
        b = beta[:, lanes]
        for h in range(heads):
            one = slice(h, h + 1)
            stack = jnp.concatenate(
                [cum[one], b[one], b[one] * grow[one], outward[one], carry[one],
                 cum[one], cum[one], cum[one]],
                axis=0,
            )
            rows_ref[h, :, lanes] = stack
            cols_ref[h, lanes, :] = jnp.transpose(stack)


def pack_terms(packs, masks_ref):
    span = PACK * BLOCK
    levels = masks_ref.shape[0] - 1
    row = lax.broadcasted_iota(jnp.int32, (span, span), 0)
    col = lax.broadcasted_iota(jnp.int32, (span, span), 1)
    strict = (row // BLOCK == col // BLOCK) & (row > col)
    prow = lax.broadcasted_iota(jnp.int32, (BLOCK, span), 0)
    pcol = lax.rem(lax.broadcasted_iota(jnp.int32, (BLOCK, span), 1), BLOCK)
    unit = prow == pcol
    couple = prow // 2 == pcol // 2
    lowers, invs, rights, outwards = [], [], [], []
    for keys, values, rows, cols in packs:
        cum_col, beta_col, pull_col, out_col = (cols[:, i : i + 1] for i in range(4))
        gram = contract(keys, keys, 1, 1)
        scale = jnp.exp(jnp.where(strict, cum_col - rows[0:1], -1e30))
        lower = (beta_col * gram) * scale
        packed = lower[0:BLOCK]
        for p in range(1, PACK):
            packed = packed + lower[p * BLOCK : (p + 1) * BLOCK]
        lowers.append(lower.astype(BF16))
        invs.append(jnp.where(unit, 1.0, jnp.where(couple, -packed, 0.0)))
        keys_f = keys.astype(F32)
        rights.append(
            jnp.concatenate(
                [(-(pull_col * keys_f)).astype(BF16), (beta_col * values).astype(BF16)], axis=1
            )
        )
        outwards.append((keys_f * out_col).astype(BF16))
    block_mask = masks_ref[levels]
    widen = lambda inv: jnp.concatenate([inv] * PACK, axis=0) * block_mask
    for level in range(levels):
        mask = masks_ref[level]
        narrow = [inv.astype(BF16) for inv in invs]
        lefts = [dot(n, lower * mask).astype(BF16) for n, lower in zip(narrow, lowers)]
        invs = [inv - dot(left, widen(n)) for inv, left, n in zip(invs, lefts, narrow)]
    fresh = [
        dot(widen(inv.astype(BF16)), right).astype(BF16) for inv, right in zip(invs, rights)
    ]
    result = []
    for (_, _, rows, _), outward, new in zip(packs, outwards, fresh):
        terms = []
        for p in range(PACK):
            block = slice(p * BLOCK, (p + 1) * BLOCK)
            carry = rows[4:5, p * BLOCK : p * BLOCK + 1]
            terms.append((carry, contract(outward[block], new[block], 0, 0)))
        result.append(terms)
    return result


def join(earlier, later):
    early_carry, early = earlier
    late_carry, late = later
    size = early.shape[0]
    grown = dot(late[:, :size].astype(BF16), early.astype(BF16))
    rest = jnp.concatenate([early_carry * late[:, :size], late[:, size:]], axis=1)
    return (early_carry * late_carry, late_carry * early + grown + rest)


def silu(array):
    half = 0.5 * array
    return half + half * jnp.tanh(half)


def segment_kernel(
    seqs, dim, first_ref, tok_ref, wk_ref, wv_ref, wgd_ref, shift_ref, rate_ref, extra_ref,
    out_ref, rows_ref, cols_ref, masks_ref, key_ref, value_ref,
):
    step = pl.program_id(0)

    @pl.when(step == 0)
    def _():
        prepare(tok_ref, wgd_ref, shift_ref, rate_ref, extra_ref, rows_ref, cols_ref, masks_ref)

    length = tok_ref.shape[0] // seqs
    per_step = wk_ref.shape[1] // dim
    span = PACK * BLOCK
    key_ref[...] = dot(tok_ref[...], wk_ref[...])
    value_ref[...] = dot(tok_ref[...], wv_ref[...])
    eye = lax.broadcasted_iota(jnp.int32, (dim, dim), 0) == lax.broadcasted_iota(
        jnp.int32, (dim, dim), 1
    )
    packs = []
    for j in range(per_step):
        head = (first_ref[0] + step) * per_step + j
        heads = slice(j * dim, (j + 1) * dim)
        for at in range(seqs * length // span):
            lanes = slice(at * span, (at + 1) * span)
            key = silu(key_ref[lanes, heads])
            key = key * lax.rsqrt(jnp.sum(key * key, axis=-1, keepdims=True) + EPS)
            value = silu(value_ref[lanes, heads]).astype(BF16).astype(F32)
            packs.append(
                (key.astype(BF16), value, rows_ref[head, :, lanes], cols_ref[head, lanes, :])
            )
    terms = pack_terms(packs, masks_ref)
    each = length // span
    chains = [
        sum(terms[i * each : (i + 1) * each], []) for i in range(per_step * seqs)
    ]
    while len(chains[0]) > 1:
        chains = [
            [join(chain[i], chain[i + 1]) for i in range(0, len(chain), 2)] for chain in chains
        ]
    for i, chain in enumerate(chains):
        carry, both = chain[0]
        out_ref[i, :, :dim] = both[:, :dim] + jnp.where(eye, carry, 0.0)
        out_ref[i, :, dim:] = both[:, dim:]


def segment_maps(
    first, some, flat, key_matrix, value_matrix, wgd, shift, rate, extra, seqs, heads, dim
):
    rows, width = flat.shape
    per_step = 2 if some % 2 == 0 else 1
    span = PACK * BLOCK
    levels = BLOCK.bit_length() - 2
    whole = lambda shape: pl.BlockSpec(shape, lambda g, first: (0,) * len(shape))
    weights = pl.BlockSpec((width, per_step * dim), lambda g, first: (0, first[0] + g))
    steps = some // per_step
    return pl.pallas_call(
        functools.partial(segment_kernel, seqs, dim),
        grid_spec=pltpu.PrefetchScalarGridSpec(
            num_scalar_prefetch=1,
            grid=(steps,),
            in_specs=[
                whole((rows, width)), weights, weights, whole(wgd.shape), whole(shift.shape),
                whole(rate.shape), whole(extra.shape),
            ],
            out_specs=pl.BlockSpec(
                (per_step * seqs, dim, 2 * dim), lambda g, first: (g, 0, 0)
            ),
            scratch_shapes=[
                pltpu.VMEM((heads, 8, rows), F32),
                pltpu.VMEM((heads, rows, 8), F32),
                pltpu.VMEM((levels + 1, span, span), BF16),
                pltpu.VMEM((rows, per_step * dim), F32),
                pltpu.VMEM((rows, per_step * dim), F32),
            ],
        ),
        out_shape=jax.ShapeDtypeStruct((some * seqs, dim, 2 * dim), F32),
        compiler_params=pltpu.CompilerParams(
            dimension_semantics=("arbitrary",), vmem_limit_bytes=56 * 1024 * 1024
        ),
        cost_estimate=pl.CostEstimate(
            flops=8 * rows * width * some * dim, transcendentals=0,
            bytes_accessed=2 * rows * width + 4 * width * some * dim,
        ),
    )(first * steps, flat, key_matrix, value_matrix, wgd, shift, rate, extra)


def token_step(final, info, gain):
    query, key, value, gate = (info[i : i + 1] for i in range(4))
    query = query * lax.rsqrt(jnp.sum(query * query, axis=-1, keepdims=True) + EPS)
    key = key * lax.rsqrt(jnp.sum(key * key, axis=-1, keepdims=True) + EPS)
    beta = 1.0 / (1.0 + jnp.exp(-gate))
    columns = jnp.transpose(jnp.concatenate([key, query, key * beta, key] + [key] * 4, axis=0))
    key_read = jnp.sum(columns[:, 0:1] * final, axis=0, keepdims=True)
    query_read = jnp.sum(columns[:, 1:2] * final, axis=0, keepdims=True)
    missing = value - key_read
    updated = final + columns[:, 2:3] * missing
    cross = jnp.sum(key * query, axis=-1, keepdims=True)
    read = (query_read + beta * cross * missing) / math.sqrt(final.shape[-1])
    read = read * lax.rsqrt(jnp.mean(read * read, axis=-1, keepdims=True) + EPS) * gain
    return updated, read


def first_pair(place, count, devices):
    start = 0
    bit = 1
    left = count
    while bit < devices:
        left //= 2
        start = start + lax.rem(place // bit, 2) * left if not isinstance(place, int) else (
            start + (place // bit) % 2 * left
        )
        bit *= 2
    return start


def merge(is_late, mine, theirs):
    dim = mine.shape[0]
    late = jnp.where(is_late, mine, theirs)
    early = jnp.where(is_late, theirs, mine)
    grown = dot3(late[:, :dim], early)
    return jnp.concatenate([grown[:, :dim], grown[:, dim:] + late[:, dim:]], axis=1)


def merge_kernel(late_ref, mine_ref, theirs_ref, out_ref):
    for i in range(mine_ref.shape[0]):
        out_ref[i] = merge(late_ref[0] == 1, mine_ref[i], theirs_ref[i])


def merge_pairs(late, mine, theirs):
    vmem = pl.BlockSpec(memory_space=pltpu.VMEM)
    count, dim, _ = mine.shape
    return pl.pallas_call(
        merge_kernel,
        in_specs=[pl.BlockSpec(memory_space=pltpu.SMEM), vmem, vmem],
        out_specs=vmem,
        out_shape=jax.ShapeDtypeStruct(mine.shape, F32),
        compiler_params=pltpu.CompilerParams(vmem_limit_bytes=16 * 1024 * 1024),
        cost_estimate=pl.CostEstimate(
            flops=12 * count * dim * dim * dim, transcendentals=0, bytes_accessed=12 * mine.size
        ),
    )(jnp.full((1,), late, jnp.int32), mine, theirs)


def exchange_kernel(
    devices, seqs, ab_ref, other_ref, next_ref, info_ref, gain_ref, state_ref, read_ref,
    got_ref, made_ref, out_buf, in_buf, read_buf, send_sem, recv_sem, put_sem, get_sem,
):
    me = lax.axis_index("sp")
    count, dim = 4 * ab_ref.shape[0], ab_ref.shape[1]
    barrier = pltpu.get_barrier_semaphore()
    for k in range(1, devices):
        pl.semaphore_signal(
            barrier, inc=1, device_id={"sp": lax.rem(me + k, devices)},
            device_id_type=pl.DeviceIdType.MESH,
        )
    pl.semaphore_wait(barrier, devices - 1)

    levels = devices.bit_length() - 1

    def halves(level):
        size = count >> (level + 1)
        bit = lax.rem(me // (1 << level), 2)
        return size, bit, bit * size, (1 - bit) * size

    def made_base(level):
        return sum(count >> i for i in range(2, level))

    def got_base(level):
        return sum(count >> i for i in range(3, level + 1))

    def order(level):
        size = count >> (level + 1)
        if level == levels - 1:
            return list(range(size))
        _, _, keep, give = halves(level + 1)
        after = order(level + 1)
        return [give + i for i in after] + [keep + i for i in after]

    def copy(level, at):
        size, bit, keep, give = halves(level)
        slot = got_base(level) + at
        return pltpu.make_async_remote_copy(
            src_ref=made_ref.at[made_base(level) + give + at], dst_ref=got_ref.at[slot],
            send_sem=send_sem.at[slot], recv_sem=recv_sem.at[slot],
            device_id={"sp": me + (1 - 2 * bit) * (1 << level)},
            device_id_type=pl.DeviceIdType.MESH,
        )

    for level in range(1, levels):
        size, bit, keep, give = halves(level)
        last = level == levels - 1
        after = [] if last else order(level + 1)
        for turn, at in enumerate(order(level)):
            if level == 1:
                mine = merge(halves(0)[1] == 1, ab_ref[at], other_ref[at])
                theirs = next_ref[at]
            else:
                copy(level, at).wait()
                mine = made_ref[made_base(level) + keep + at]
                theirs = got_ref[got_base(level) + at]
            if last:
                is_late = bit == 1
                late = jnp.where(is_late, mine, theirs)
                early = jnp.where(is_late, theirs, mine)
                final = dot3(late[:, :dim], early[:, dim:]) + late[:, dim:]
                pair = first_pair(me, count, devices) + at
                updated, read = token_step(final, info_ref[pair], gain_ref[...])
                out_buf[:, at, : dim // devices, :] = updated.reshape(devices, dim // devices, dim)
                out_buf[:, at, dim // devices :, :] = jnp.broadcast_to(read, (devices, 8, dim))
            else:
                made_ref[made_base(level + 1) + at] = merge(bit == 1, mine, theirs)
                if turn < len(after):
                    copy(level + 1, after[turn]).start()

    def put(k):
        dest = lax.rem(me + k, devices)
        return pltpu.make_async_remote_copy(
            src_ref=out_buf.at[dest], dst_ref=in_buf.at[me],
            send_sem=put_sem.at[k], recv_sem=get_sem.at[k],
            device_id={"sp": dest}, device_id_type=pl.DeviceIdType.MESH,
        )

    for k in range(1, devices):
        put(k).start()
    in_buf[me] = out_buf[me]
    for k in range(1, devices):
        put(k).wait()
    own = count // devices
    rows = dim // devices
    for e in range(devices):
        for i in range(own):
            pair = first_pair(e, count, devices) + i
            h, s = pair // seqs, pair % seqs
            state_ref[s, h] = in_buf[e, i, :rows, :].astype(BF16)
            read_buf[s, h : h + 1, :] = in_buf[e, i, rows : rows + 1, :]
    read_ref[...] = read_buf[...].astype(BF16)


def exchange(ab, other, following, info, gain, seqs, heads, devices):
    count, dim = 4 * ab.shape[0], ab.shape[1]
    slots = count // 4 - count // devices
    vmem = pl.BlockSpec(memory_space=pltpu.VMEM)
    return pl.pallas_call(
        functools.partial(exchange_kernel, devices, seqs),
        in_specs=[vmem] * 5,
        out_specs=[vmem] * 2,
        out_shape=[
            jax.ShapeDtypeStruct((seqs, heads, dim // devices, dim), BF16),
            jax.ShapeDtypeStruct((seqs, heads, dim), BF16),
        ],
        scratch_shapes=[
            pltpu.VMEM((slots, dim, 2 * dim), F32),
            pltpu.VMEM((slots + count // devices + count // 4, dim, 2 * dim), F32),
            pltpu.VMEM((devices, count // devices, dim // devices + 8, dim), F32),
            pltpu.VMEM((devices, count // devices, dim // devices + 8, dim), F32),
            pltpu.VMEM((seqs, heads, dim), F32),
            pltpu.SemaphoreType.DMA((slots,)),
            pltpu.SemaphoreType.DMA((slots,)),
            pltpu.SemaphoreType.DMA((devices,)),
            pltpu.SemaphoreType.DMA((devices,)),
        ],
        compiler_params=pltpu.CompilerParams(
            collective_id=0, has_side_effects=True, vmem_limit_bytes=16 * 1024 * 1024
        ),
    )(ab, other, following, info, gain)


def gathered_exchange(ab, info, gain, seqs, heads, devices):
    count, dim = ab.shape[0], ab.shape[1]
    everyone = lax.all_gather(ab, "sp")

    def one(at, state):
        step = lax.dynamic_index_in_dim(everyone, at, 0, False)
        return (
            jnp.matmul(step[..., :dim], state, precision=lax.Precision.HIGHEST) + step[..., dim:]
        )

    final = lax.fori_loop(0, devices, one, jnp.zeros((count, dim, dim), F32))
    updated, read = jax.vmap(lambda f, i: token_step(f, i, gain))(final, info)
    rows = dim // devices
    mine = lax.dynamic_slice_in_dim(updated, lax.axis_index("sp") * rows, rows, 1)
    mine = jnp.swapaxes(mine.reshape(heads, seqs, rows, dim), 0, 1)
    return mine.astype(BF16), jnp.swapaxes(read.reshape(heads, seqs, dim), 0, 1).astype(BF16)


def shards(
    tokens, key_matrix, value_matrix, gate_matrix, decay_matrix, gate_bias_offset,
    head_log_decay_rate, extra_log_decay, next_token_query, next_token_key,
    next_token_value, next_token_gate, readout_norm_gain,
):
    seqs, length, width = tokens.shape
    dim = next_token_key.shape[-1]
    heads = key_matrix.shape[1] // dim
    devices = lax.axis_size("sp")
    first = lax.axis_index("tp") * heads
    flat = tokens.reshape(seqs * length, width)
    pick = lambda array, axis: lax.dynamic_slice_in_dim(array, first, heads, axis)
    wgd = jnp.concatenate([pick(gate_matrix, 1), pick(decay_matrix, 1)], axis=1).T
    shift = pick(gate_bias_offset, 0)[:, None]
    rate = pick(head_log_decay_rate, 0)[:, None]
    extra = extra_log_decay.reshape(seqs * length, heads).T
    wide = lambda array: jnp.swapaxes(array.astype(F32), 0, 1).reshape(heads * seqs, 1, dim)
    gate = jnp.broadcast_to(next_token_gate[..., None], next_token_key.shape)
    info = jnp.concatenate(
        [wide(next_token_query), wide(next_token_key), wide(next_token_value), wide(gate)], axis=1
    )
    gain = readout_norm_gain[None, :]
    maps = lambda at, some, flat=flat: segment_maps(
        jnp.full((1,), at, jnp.int32), some, flat, key_matrix, value_matrix, wgd, shift, rate,
        extra, seqs, heads, dim,
    )
    paired = devices & (devices - 1) == 0 and devices > 4 and heads % 4 == 0
    if not paired or (seqs * heads) % devices:
        return gathered_exchange(maps(0, heads), info, gain, seqs, heads, devices)
    place = lax.axis_index("sp")
    late, later = lax.rem(place, 2), lax.rem(place // 2, 2)
    swap = lambda array, step: lax.ppermute(array, "sp", [(i, i ^ step) for i in range(devices)])
    quarter = heads // 4
    other_first = swap(maps(2 * (1 - late) + 1 - later, quarter), 1)
    other = swap(maps(2 * (1 - late) + later, quarter), 1)
    merged = merge_pairs(late, maps(2 * late + 1 - later, quarter), other_first)
    flat, merged = lax.optimization_barrier((flat, merged))
    following = swap(merged, 2)
    kept = maps(2 * late + later, quarter, flat)
    return exchange(kept, other, following, info, gain, seqs, heads, devices)


def solution(mesh):
    return jax.shard_map(
        shards,
        mesh=mesh,
        in_specs=(
            P("gr", "sp", None), P(None, "tp"), P(None, "tp"), P(), P(), P(), P(),
            P("gr", "sp", "tp"), P("gr", "tp", None), P("gr", "tp", None),
            P("gr", "tp", None), P("gr", "tp"), P(),
        ),
        out_specs=(P("gr", "tp", "sp", None), P("gr", "tp", None)),
        check_vma=False,
    )
```
